32 devices in a mesh: sp: 8 (over z, y), tp: 4 (over x, core).
Axes of the slice: x: 2, y: 2, z: 4, core: 2. Of those that a mesh axis runs over, the one named last changes fastest.
Arguments:
- tokens: bfloat16 [2048, 4096], P(('sp', 'tp')), may hold values from -700 to 700
- down_query: bfloat16 [4096, 1024], replicated, may hold values from -0.09375 to 0.09375
- down_latent: bfloat16 [4096, 512], replicated, may hold values from -0.09375 to 0.09375
- down_rotary: bfloat16 [4096, 64], replicated, may hold values from -0.09375 to 0.09375
- query_gain: float32 [1024], replicated, may hold values from 0.1 to 1.9
- latent_gain: float32 [512], replicated, may hold values from 0.1 to 1.9
- up_query: bfloat16 [1024, 2048], P(None, 'tp'), may hold values from -0.1875 to 0.1875
- up_query_rotary: bfloat16 [1024, 1024], P(None, 'tp'), may hold values from -0.1875 to 0.1875
- up_key: bfloat16 [512, 2048], P(None, 'tp'), may hold values from -0.25 to 0.25
- up_value: bfloat16 [512, 2048], P(None, 'tp'), may hold values from -0.25 to 0.25
- out_weight: bfloat16 [2048, 4096], P('tp'), may hold values from -0.39648438 to 0.39648438
Outputs:
- mixed: bfloat16 [2048, 4096], P(('sp', 'tp'))
The draws below stay inside these ranges and needn't reach their ends.
All inputs are finite; a program needn't handle non-finite values.
Results may differ from the reference program's by a relative error of at most 0.03.
Values may be sent and summed in bfloat16 or wider, within the bound.
A program may use at most 192 MiB of HBM per device.

```python
import jax
import jax.numpy as jnp
from jax import lax

D = 4096
HEADS = 16
NOPE = 128
ROPE = 64
VDIM = 128
QRANK = 1024
KVRANK = 512
TOK_DEV = 256
TOKENS = 2048
N_TP = 4


def draw_tokens(key, part):
    first_key, second_key, third_key = jax.random.split(jax.random.fold_in(key, 11), 3)
    offsets = jax.random.normal(second_key, (TOKENS // TOK_DEV, D), jnp.float32) * 0.7
    shifted = jnp.repeat(offsets, TOK_DEV, axis=0)
    rough = jax.random.normal(first_key, (TOKENS, D), jnp.float32) + shifted
    return jnp.clip(rough, -700.0, 700.0).astype(jnp.bfloat16)


def shard_levels(stream_key, dims, cuts, smallest, high):
    loudness, own = 1.0, jax.random.fold_in(stream_key, 6)
    for dim, parts in cuts:
        heights = jnp.exp(jax.random.uniform(jax.random.fold_in(own, dim), (parts,), jnp.float32, smallest / len(cuts), high / len(cuts)))
        loudness = loudness * jnp.repeat(heights, dims[dim] // parts).reshape([-1 if axis == dim else 1 for axis in range(len(dims))])
    return loudness


def normal_values(rng, shape, width, bound, pieces=(), held_as=jnp.bfloat16):
    values = jax.random.normal(rng, shape, jnp.float32) * width
    if len(pieces) > 0:
        values = shard_levels(rng, shape, pieces, -0.22, 0.18) * values
    return jnp.clip(values, min=-bound, max=bound).astype(held_as)


def setup_inputs(seed: int = 0) -> dict:
    splits = jax.random.split(jax.random.key(seed), 12)
    tokens = draw_tokens(jax.random.fold_in(splits[11], 71), 0)
    down_query = normal_values(splits[1], (D, QRANK), D ** -0.5, 0.09375)
    down_latent = normal_values(splits[2], (D, KVRANK), D ** -0.5, 0.09375)
    down_rotary = normal_values(splits[3], (D, ROPE), D ** -0.5, 0.09375)
    query_gain = jnp.clip(1.0 + 0.18 * jax.random.normal(splits[4], (QRANK,), jnp.float32), 0.1, 1.9)
    latent_gain = jnp.clip(1.0 + 0.18 * jax.random.normal(splits[5], (KVRANK,), jnp.float32), 0.1, 1.9)
    up_query = normal_values(splits[6], (QRANK, HEADS * NOPE), QRANK ** -0.5, 0.1875, ((1, 4),))
    up_query_rotary = normal_values(splits[7], (QRANK, HEADS * ROPE), QRANK ** -0.5, 0.1875, ((1, 4),))
    up_key = normal_values(splits[8], (KVRANK, HEADS * NOPE), KVRANK ** -0.5, 0.25, ((1, 4),))
    up_value = normal_values(splits[9], (KVRANK, HEADS * VDIM), KVRANK ** -0.5, 0.25, ((1, 4),))
    out_weight = normal_values(splits[10], (HEADS * VDIM, D), (3.0 * (HEADS * VDIM) ** -0.5), 0.39648438, ((0, 4),))
    return dict(tokens=tokens, down_query=down_query, down_latent=down_latent, down_rotary=down_rotary, query_gain=query_gain, latent_gain=latent_gain, up_query=up_query, up_query_rotary=up_query_rotary, up_key=up_key, up_value=up_value, out_weight=out_weight)


rope_base = 500000.0
norm_eps = 1e-06
masked_score = -1e+30

def rotate_half(values, positions):
    half = values.shape[-1] // 2
    inverse = rope_base ** (-jnp.arange(0, 2 * half, 2, dtype=jnp.float32) / (2 * half))
    angles = positions.astype(jnp.float32)[:, None] * inverse
    if values.ndim == 3:
        angles = angles[:, None, :]
    cosine = jnp.cos(angles)
    sine = jnp.sin(angles)
    first = values[..., :half]
    second = values[..., half:]
    return jnp.concatenate([first * cosine - second * sine, second * cosine + first * sine], axis=-1)

def norm_rows(values, gain):
    return values * lax.rsqrt(lax.optimization_barrier(jnp.mean(values * values, axis=-1, keepdims=True)) + norm_eps) * gain

def reference(tokens, down_query, down_latent, down_rotary, query_gain, latent_gain, up_query, up_query_rotary, up_key, up_value, out_weight):
    positions = jnp.arange(TOKENS, dtype=jnp.int32)
    query_latent = norm_rows(jnp.dot(tokens, down_query, preferred_element_type=jnp.float32), query_gain).astype(jnp.bfloat16)
    kv_latent = norm_rows(jnp.dot(tokens, down_latent, preferred_element_type=jnp.float32), latent_gain).astype(jnp.bfloat16)
    key_rotary = rotate_half(jnp.dot(tokens, down_rotary, preferred_element_type=jnp.float32), positions).astype(jnp.bfloat16)
    query_plain = jnp.dot(query_latent, up_query, preferred_element_type=jnp.float32).astype(jnp.bfloat16).reshape(TOKENS, HEADS, NOPE)
    query_turned = rotate_half(jnp.dot(query_latent, up_query_rotary, preferred_element_type=jnp.float32).reshape(TOKENS, HEADS, ROPE), positions).astype(jnp.bfloat16)
    key_plain = jnp.dot(kv_latent, up_key, preferred_element_type=jnp.float32).astype(jnp.bfloat16).reshape(TOKENS, HEADS, NOPE)
    values = jnp.dot(kv_latent, up_value, preferred_element_type=jnp.float32).astype(jnp.bfloat16).reshape(TOKENS, HEADS, VDIM)
    factor = (NOPE + ROPE) ** (-0.5)
    block = 512 if TOKENS % 512 == 0 else TOKENS
    outputs = []
    for first in range(0, TOKENS, block):
        stop = first + block
        scores = jnp.einsum('qhd,khd->hqk', query_plain[first:stop].astype(jnp.float32), key_plain[:stop].astype(jnp.float32))
        scores = scores + jnp.einsum('qhr,kr->hqk', query_turned[first:stop].astype(jnp.float32), key_rotary[:stop].astype(jnp.float32))
        scores = scores * factor
        allowed = (positions[:stop][None, :] <= positions[first:stop][:, None])[None]
        scores = jnp.where(allowed, scores, masked_score)
        best = lax.optimization_barrier(jnp.max(scores, axis=-1, keepdims=True))
        weights = jnp.where(allowed, jnp.exp(scores - best), 0.0)
        total = lax.optimization_barrier(jnp.sum(weights, axis=-1))
        rounded = lax.optimization_barrier(weights.astype(jnp.bfloat16)).astype(jnp.float32)
        summed = jnp.einsum('hqk,khd->qhd', rounded, values[:stop].astype(jnp.float32))
        outputs.append((summed / jnp.transpose(total)[:, :, None]).astype(jnp.bfloat16).reshape(block, HEADS * VDIM))
    attended = jnp.concatenate(outputs, axis=0)
    group_width = HEADS * VDIM // N_TP
    mixed = jnp.zeros((TOKENS, D), jnp.float32)
    for group in range(N_TP):
        lower = group * group_width
        partial_sum = jnp.dot(attended[:, lower:lower + group_width], out_weight[lower:lower + group_width], preferred_element_type=jnp.float32)
        mixed = mixed + lax.optimization_barrier(partial_sum.astype(jnp.bfloat16)).astype(jnp.float32)
    return mixed.astype(jnp.bfloat16)
```

```python
import functools

import jax
import jax.numpy as jnp
from jax import lax
from jax.experimental import pallas as pl
from jax.experimental.pallas import tpu as pltpu
from jax.sharding import PartitionSpec as P

NOPE = 128
ROPE = 64
VDIM = 128
LANES = 128

rope_base = 500000.0
norm_eps = 1e-06
masked_score = -1e30
log2e = 1.4426950408889634

MESH = pl.DeviceIdType.MESH
F32 = jnp.float32
BF16 = jnp.bfloat16


def dot(a, b):
    return jnp.dot(a, b, preferred_element_type=F32)


def turn(v, cosine, sine):
    lane = lax.broadcasted_iota(jnp.int32, v.shape, 1)
    other = jnp.where(lane % ROPE < ROPE // 2, pltpu.roll(v, LANES - ROPE // 2, 1), pltpu.roll(v, ROPE // 2, 1))
    return v * cosine + other * sine


def normed(v, gain):
    return v * lax.rsqrt(jnp.mean(v * v, axis=-1, keepdims=True) + norm_eps) * gain


def kernel(
    S,
    T,
    chunks,
    pieces,
    tokens_hbm,
    dq_hbm,
    dl_hbm,
    dr_hbm,
    qg_ref,
    lg_ref,
    uq_hbm,
    ur_hbm,
    uk_hbm,
    uv_hbm,
    ow_hbm,
    cos_ref,
    sin_ref,
    out_ref,
    tokens,
    dq,
    dl,
    dr,
    uq,
    ur,
    uk,
    uv,
    ow,
    kv,
    ql,
    qh,
    acc,
    best,
    att,
    pair_out,
    pair_in,
    kept,
    cross_out,
    cross_in,
    load_sem,
    kv_send,
    kv_recv,
    q_send,
    q_recv,
    pair_send,
    pair_recv,
    cross_send,
    cross_recv,
):
    O = S // 2
    rows = tokens.shape[0]
    span = rows * T
    depth = tokens.shape[1]
    heads = qh.shape[0]
    rank = dl.shape[1]
    sp = lax.axis_index("sp")
    tp = lax.axis_index("tp")
    o, i = sp // 2, sp % 2
    g, c = tp // 2, tp % 2

    def dev(o_, i_, g_, c_):
        return {"sp": o_ * 2 + i_, "tp": g_ * 2 + c_}

    across = dev(o, i, 1 - g, c)
    beside = dev(o, 1 - i, g, c)
    mate = dev(o, i, g, 1 - c)

    step = depth // chunks
    loads = []

    def load(src, dst):
        copy = pltpu.make_async_copy(src, dst, load_sem.at[len(loads)])
        loads.append(copy)
        copy.start()
        return copy

    tok_load = load(tokens_hbm, tokens)
    dl_loads = [load(dl_hbm.at[pl.ds(k * step, step)], dl.at[pl.ds(k * step, step)]) for k in range(chunks)]
    dr_load = load(dr_hbm, dr)
    dq_loads = [load(dq_hbm.at[pl.ds(k * step, step)], dq.at[pl.ds(k * step, step)]) for k in range(chunks)]
    up_loads = [load(uq_hbm, uq), load(ur_hbm, ur), load(uk_hbm, uk), load(uv_hbm, uv)]
    ow_load = load(ow_hbm, ow)

    barrier = pltpu.get_barrier_semaphore()
    for d in range(1, O):
        pl.semaphore_signal(barrier, inc=1, device_id=dev((o + d) % O, i, g, c), device_id_type=MESH)
    for target in (across, beside, mate):
        pl.semaphore_signal(barrier, inc=1, device_id=target, device_id_type=MESH)

    def block(o_, i_, g_, c_):
        return (o_ * 2 + i_) * T + g_ * 2 + c_

    def block_rows(b):
        return pl.ds(pl.multiple_of(b * rows, rows), rows)

    def kv_copy(b, target, index):
        part = kv.at[block_rows(b)]
        return pltpu.make_async_remote_copy(
            src_ref=part,
            dst_ref=part,
            send_sem=kv_send.at[index],
            recv_sem=kv_recv.at[b],
            device_id=target,
            device_id_type=MESH,
        )

    def kv_wait(b):
        kv_copy(b, mate, 0).wait_recv()

    tok_load.wait()
    latent = jnp.zeros((rows, rank), F32)
    for k in range(chunks):
        dl_loads[k].wait()
        latent += dot(tokens[:, k * step : (k + 1) * step], dl[k * step : (k + 1) * step, :])
    dr_load.wait()
    turned = dot(tokens[...], dr[...])
    turned = jnp.concatenate([turned, jnp.zeros((rows, LANES - ROPE), F32)], axis=1)
    own_rows = pl.ds(pl.multiple_of(tp * rows, rows), rows)
    mine = block_rows(block(o, i, g, c))
    kv[mine, :rank] = normed(latent, lg_ref[...]).astype(BF16)
    kv[mine, rank:] = turn(turned, cos_ref[own_rows, :], sin_ref[own_rows, :]).astype(BF16)

    pl.semaphore_wait(barrier, O - 1 + 3)

    def up_copy(d):
        return kv_copy(block(o, i, g, c), dev((o + d) % O, i, g, c), d)

    def relay_near(d, act):
        b = block(o - d, i, g, c)
        act(kv_copy(b, across, O + d))

        @pl.when((i == 0) | (d > 0))
        def _():
            act(kv_copy(b, beside, 2 * O + 2 * d))

        act(kv_copy(b, mate, 4 * O + 4 * d))

    def relay_far(d, act):
        b = block(o - d, i, 1 - g, c)

        @pl.when((i == 0) | (d > 0))
        def _():
            act(kv_copy(b, beside, 2 * O + 2 * d + 1))

        act(kv_copy(b, mate, 4 * O + 4 * d + 1))

    def relay_beside(d, act):
        act(kv_copy(block(o - d, 1 - i, g, c), mate, 4 * O + 4 * d + 2))
        act(kv_copy(block(o - d, 1 - i, 1 - g, c), mate, 4 * O + 4 * d + 3))

    def start(copy):
        copy.start()

    def sent(copy):
        copy.wait_send()

    def relay(d):
        kv_wait(block(o - d, i, g, c))
        relay_near(d, start)
        kv_wait(block(o - d, i, 1 - g, c))
        relay_far(d, start)

    for d in range(1, O):

        @pl.when(o + d < O)
        def _(d=d):
            up_copy(d).start()

    relay_near(0, start)

    query = jnp.zeros((rows, dq.shape[1]), F32)
    for k in range(chunks):
        dq_loads[k].wait()
        query += dot(tokens[:, k * step : (k + 1) * step], dq[k * step : (k + 1) * step, :])
        if k == chunks // 2 - 1:
            kv_wait(block(o, i, 1 - g, c))
            relay_far(0, start)
    ql[own_rows, :] = normed(query, qg_ref[...]).astype(BF16)

    def q_copy(t, target, index):
        part = ql.at[block_rows(t)]
        return pltpu.make_async_remote_copy(
            src_ref=part,
            dst_ref=part,
            send_sem=q_send.at[index],
            recv_sem=q_recv.at[t],
            device_id=target,
            device_id_type=MESH,
        )

    far = (1 - g) * 2 + c
    q_copies = [q_copy(tp, across, 0), q_copy(tp, mate, 1), q_copy(far, mate, 2)]
    q_copies[0].start()
    q_copies[1].start()

    @pl.when(o >= 1)
    def _():
        relay(1)

    q_copy(far, mate, 2).wait_recv()
    q_copies[2].start()
    q_copy(g * 2 + 1 - c, mate, 0).wait_recv()
    q_copy((1 - g) * 2 + 1 - c, mate, 0).wait_recv()

    for copy in up_loads:
        copy.wait()
    plain = dot(ql[...], uq[...]).astype(BF16)
    turning = dot(ql[...], ur[...])
    low = lax.broadcasted_iota(jnp.int32, (span, LANES), 1) < ROPE
    for pair in range(heads // 2):
        both = turn(turning[:, pair * LANES : (pair + 1) * LANES], cos_ref[...], sin_ref[...])
        qh[2 * pair, :, NOPE:] = jnp.where(low, both, 0.0).astype(BF16)
        qh[2 * pair + 1, :, NOPE:] = jnp.where(low, pltpu.roll(both, ROPE, 1), 0.0).astype(BF16)
    for h in range(heads):
        qh[h, :, :NOPE] = plain[:, h * NOPE : (h + 1) * NOPE]
        best[h] = jnp.full((span, LANES), masked_score, F32)
        acc[h] = jnp.zeros((span, 2 * VDIM), F32)

    scale = (NOPE + ROPE) ** (-0.5) * log2e

    def attend(s):
        part = pl.ds(pl.multiple_of(s * span, span), span)
        lat = kv[part, :rank]
        rot = kv[part, rank:]
        keys = dot(lat, uk[...]).astype(BF16)
        values = dot(lat, uv[...]).astype(BF16)
        ones = jnp.ones((span, VDIM), BF16)
        q_pos = sp * span + lax.broadcasted_iota(jnp.int32, (span, span), 0)
        k_pos = s * span + lax.broadcasted_iota(jnp.int32, (span, span), 1)
        allowed = k_pos <= q_pos
        for h in range(heads):
            key = jnp.concatenate([keys[:, h * NOPE : (h + 1) * NOPE], rot], axis=1)
            value = jnp.concatenate([values[:, h * VDIM : (h + 1) * VDIM], ones], axis=1)
            scores = lax.dot_general(qh[h], key, (((1,), (1,)), ((), ())), preferred_element_type=F32)
            scores = jnp.where(allowed, scores * scale, masked_score)
            old = best[h][:, :1]
            new = jnp.maximum(old, jnp.max(scores, axis=-1, keepdims=True))
            weights = jnp.exp2(scores - new).astype(BF16)
            acc[h] = acc[h] * jnp.exp2(old - new) + dot(weights, value)
            best[h] = jnp.broadcast_to(new, (span, LANES))

    def visit(d, carry):
        @pl.when(d + 2 <= o)
        def _():
            relay(d + 2)

        kv_wait(block(o - d, i, g, 1 - c))
        kv_wait(block(o - d, i, 1 - g, 1 - c))
        attend((o - d) * 2 + i)

        @pl.when((i == 1) | (d > 0))
        def _():
            kv_wait(block(o - d, 1 - i, g, c))
            kv_wait(block(o - d, 1 - i, 1 - g, c))
            relay_beside(d, start)
            kv_wait(block(o - d, 1 - i, g, 1 - c))
            kv_wait(block(o - d, 1 - i, 1 - g, 1 - c))
            attend((o - d) * 2 + 1 - i)

        return carry

    lax.fori_loop(0, o + 1, visit, 0)

    for h in range(heads):
        whole = acc[h]
        att[:, h * VDIM : (h + 1) * VDIM] = (whole[:, :VDIM] / whole[:, VDIM:]).astype(BF16)

    ow_load.wait()
    width = ow.shape[1] // pieces

    def pair_copy(phase, j):
        return pltpu.make_async_remote_copy(
            src_ref=pair_out.at[phase, j],
            dst_ref=pair_in.at[phase, j],
            send_sem=pair_send.at[phase * pieces + j],
            recv_sem=pair_recv.at[phase * pieces + j],
            device_id=mate,
            device_id_type=MESH,
        )

    def cross_copy(j):
        return pltpu.make_async_remote_copy(
            src_ref=cross_out.at[j],
            dst_ref=cross_in.at[j],
            send_sem=cross_send.at[j],
            recv_sem=cross_recv.at[j],
            device_id=across,
            device_id_type=MESH,
        )

    def project(phase, group, j):
        top = att[block_rows(group * 2 + 1 - c), :]
        low_part = att[block_rows(group * 2 + c), :]
        part = dot(jnp.concatenate([top, low_part], axis=0), ow[:, j * width : (j + 1) * width])
        pair_out[phase, j] = part[:rows].astype(BF16)
        kept[phase, j] = part[rows:]
        pair_copy(phase, j).start()

    def cross(j):
        pair_copy(0, j).wait_recv()
        cross_out[j] = (kept[0, j] + pair_in[0, j].astype(F32)).astype(BF16)
        cross_copy(j).start()

    for j in range(pieces):
        project(0, 1 - g, j)
        if j >= 3:
            cross(j - 3)
    for j in range(pieces - 3, pieces):
        cross(j)
    for j in range(pieces):
        project(1, g, j)
    for j in range(pieces):
        pair_copy(1, j).wait_recv()
        cross_copy(j).wait_recv()
        total = kept[1, j] + pair_in[1, j].astype(F32) + cross_in[j].astype(F32)
        out_ref[:, j * width : (j + 1) * width] = total.astype(BF16)

    for d in range(1, O):

        @pl.when(o + d < O)
        def _(d=d):
            up_copy(d).wait_send()

    def drain(d, carry):
        relay_near(d, sent)
        relay_far(d, sent)

        @pl.when((i == 1) | (d > 0))
        def _():
            relay_beside(d, sent)

        return carry

    lax.fori_loop(0, o + 1, drain, 0)
    for copy in q_copies:
        copy.wait_send()
    for j in range(pieces):
        pair_copy(0, j).wait_send()
        pair_copy(1, j).wait_send()
        cross_copy(j).wait_send()


def solution(mesh):
    S, T = mesh.shape["sp"], mesh.shape["tp"]
    assert S % 2 == 0 and T == 4

    def local(tokens, dq, dl, dr, qg, lg, uq, ur, uk, uv, ow):
        rows, depth = tokens.shape
        span = rows * T
        heads = uk.shape[1] // NOPE
        width = ow.shape[1]
        rank = dl.shape[1]
        half = ROPE // 2
        chunks, pieces = 4, 8
        inverse = rope_base ** (-jnp.arange(0, ROPE, 2, dtype=F32) / ROPE)
        positions = lax.axis_index("sp") * span + jnp.arange(span, dtype=jnp.int32)
        angles = positions.astype(F32)[:, None] * jnp.tile(inverse, LANES // half)
        sign = jnp.where(jnp.arange(LANES) % ROPE < half, -1.0, 1.0).astype(F32)
        cosine = jnp.cos(angles)
        sine = jnp.sin(angles) * sign
        O = S // 2
        hbm = pl.BlockSpec(memory_space=pl.ANY)
        vmem = pl.BlockSpec(memory_space=pltpu.VMEM)
        dma = lambda n: pltpu.SemaphoreType.DMA((n,))
        like = lambda a: pltpu.VMEM(a.shape, a.dtype)
        return pl.pallas_call(
            functools.partial(kernel, S, T, chunks, pieces),
            out_shape=jax.ShapeDtypeStruct((rows, width), BF16),
            in_specs=[hbm, hbm, hbm, hbm, vmem, vmem, hbm, hbm, hbm, hbm, hbm, vmem, vmem],
            out_specs=vmem,
            scratch_shapes=[
                like(tokens),
                like(dq),
                like(dl),
                like(dr),
                like(uq),
                like(ur),
                like(uk),
                like(uv),
                like(ow),
                pltpu.VMEM((S * span, rank + LANES), BF16),
                pltpu.VMEM((span, dq.shape[1]), BF16),
                pltpu.VMEM((heads, span, NOPE + LANES), BF16),
                pltpu.VMEM((heads, span, 2 * VDIM), F32),
                pltpu.VMEM((heads, span, LANES), F32),
                pltpu.VMEM((span, heads * VDIM), BF16),
                pltpu.VMEM((2, pieces, rows, width // pieces), BF16),
                pltpu.VMEM((2, pieces, rows, width // pieces), BF16),
                pltpu.VMEM((2, pieces, rows, width // pieces), F32),
                pltpu.VMEM((pieces, rows, width // pieces), BF16),
                pltpu.VMEM((pieces, rows, width // pieces), BF16),
                dma(2 * chunks + 7),
                dma(8 * O),
                dma(S * T),
                dma(3),
                dma(T),
                dma(2 * pieces),
                dma(2 * pieces),
                dma(pieces),
                dma(pieces),
            ],
            compiler_params=pltpu.CompilerParams(
                collective_id=0, has_side_effects=True, vmem_limit_bytes=60 * 1024 * 1024
            ),
        )(
            tokens, dq, dl, dr, qg.reshape(1, -1), lg.reshape(1, -1),
            uq, ur, uk, uv, ow, cosine, sine,
        )

    return jax.shard_map(
        local,
        mesh=mesh,
        in_specs=(
            P(("sp", "tp"), None),
            P(),
            P(),
            P(),
            P(),
            P(),
            P(None, "tp"),
            P(None, "tp"),
            P(None, "tp"),
            P(None, "tp"),
            P("tp", None),
        ),
        out_specs=P(("sp", "tp"), None),
        check_vma=False,
    )
```

```python
import functools

import jax
import jax.numpy as jnp
import numpy as np
from jax import lax
from jax.experimental import pallas as pl
from jax.experimental.pallas import tpu as pltpu
from jax.sharding import PartitionSpec as P

NOPE = 128
ROPE = 64
VDIM = 128
LANES = 128

rope_base = 500000.0
norm_eps = 1e-06
masked_score = -1e30
log2e = 1.4426950408889634

MESH = pl.DeviceIdType.MESH
F32 = jnp.float32
BF16 = jnp.bfloat16


def dot(a, b):
    return jnp.dot(a, b, preferred_element_type=F32)


def dot_nt(a, b):
    return lax.dot_general(a, b, (((1,), (1,)), ((), ())), preferred_element_type=F32)


def turn(v, cosine, sine):
    lane = lax.broadcasted_iota(jnp.int32, v.shape, 1)
    other = jnp.where(lane % ROPE < ROPE // 2, pltpu.roll(v, LANES - ROPE // 2, 1), pltpu.roll(v, ROPE // 2, 1))
    return v * cosine + other * sine


def normed(v, gain):
    return v * lax.rsqrt(jnp.mean(v * v, axis=-1, keepdims=True) + norm_eps) * gain


def kernel(
    S,
    T,
    chunks,
    pieces,
    tokens_hbm,
    dq_hbm,
    dl_hbm,
    dr_hbm,
    qg_ref,
    lg_ref,
    uq_hbm,
    ur_hbm,
    uk_hbm,
    uv_hbm,
    ow_hbm,
    base_cos,
    base_sin,
    row_cos,
    row_sin,
    out_ref,
    tokens,
    dq,
    dl,
    dr,
    uq,
    ur,
    uk,
    uv,
    ow,
    kv,
    ql,
    qh,
    acc,
    best,
    att,
    pair_out,
    pair_in,
    kept,
    cross_out,
    cross_in,
    uvt,
    cos_ref,
    sin_ref,
    load_sem,
    kv_send,
    kv_recv,
    q_send,
    q_recv,
    pair_send,
    pair_recv,
    cross_send,
    cross_recv,
):
    O = S // 2
    rows = tokens.shape[0]
    span = rows * T
    depth = tokens.shape[1]
    heads = qh.shape[0]
    rank = dl.shape[1]
    sp = lax.axis_index("sp")
    tp = lax.axis_index("tp")
    o, i = sp // 2, sp % 2
    g, c = tp // 2, tp % 2

    def dev(o_, i_, g_, c_):
        return {"sp": o_ * 2 + i_, "tp": g_ * 2 + c_}

    across = dev(o, i, 1 - g, c)
    beside = dev(o, 1 - i, g, c)
    mate = dev(o, i, g, 1 - c)

    step = depth // chunks
    loads = []

    def load(src, dst):
        copy = pltpu.make_async_copy(src, dst, load_sem.at[len(loads)])
        loads.append(copy)
        copy.start()
        return copy

    tok_load = load(tokens_hbm, tokens)
    dl_loads = [load(dl_hbm.at[pl.ds(k * step, step)], dl.at[pl.ds(k * step, step)]) for k in range(chunks)]
    dr_load = load(dr_hbm, dr)
    dq_loads = [load(dq_hbm.at[pl.ds(k * step, step)], dq.at[pl.ds(k * step, step)]) for k in range(chunks)]
    up_loads = [load(uq_hbm, uq), load(ur_hbm, ur), load(uk_hbm, uk), load(uv_hbm, uv)]
    ow_load = load(ow_hbm, ow)

    barrier = pltpu.get_barrier_semaphore()
    for d in range(1, O):
        pl.semaphore_signal(barrier, inc=1, device_id=dev((o + d) % O, i, g, c), device_id_type=MESH)
    for target in (across, beside, mate):
        pl.semaphore_signal(barrier, inc=1, device_id=target, device_id_type=MESH)

    def block(o_, i_, g_, c_):
        return (o_ * 2 + i_) * T + g_ * 2 + c_

    def block_rows(b):
        return pl.ds(pl.multiple_of(b * rows, rows), rows)

    def kv_copy(b, target, index):
        part = kv.at[block_rows(b)]
        return pltpu.make_async_remote_copy(
            src_ref=part,
            dst_ref=part,
            send_sem=kv_send.at[index],
            recv_sem=kv_recv.at[b],
            device_id=target,
            device_id_type=MESH,
        )

    def kv_wait(b):
        kv_copy(b, mate, 0).wait_recv()

    start_cos, start_sin = base_cos[pl.ds(sp, 1), :], base_sin[pl.ds(sp, 1), :]
    sign = jnp.where(lax.broadcasted_iota(jnp.int32, (1, LANES), 1) % ROPE < ROPE // 2, -1.0, 1.0)
    cos_ref[...] = start_cos * row_cos[...] - start_sin * row_sin[...]
    sin_ref[...] = (start_sin * row_cos[...] + start_cos * row_sin[...]) * sign

    tok_load.wait()
    latent = jnp.zeros((rows, rank), F32)
    for k in range(chunks):
        dl_loads[k].wait()
        latent += dot(tokens[:, k * step : (k + 1) * step], dl[k * step : (k + 1) * step, :])
    dr_load.wait()
    turned = dot_nt(tokens[...], dr[...])
    turned = jnp.concatenate([turned, jnp.zeros((rows, LANES - ROPE), F32)], axis=1)
    own_rows = pl.ds(pl.multiple_of(tp * rows, rows), rows)
    mine = block_rows(block(o, i, g, c))
    kv[mine, :rank] = normed(latent, lg_ref[...]).astype(BF16)
    kv[mine, rank:] = turn(turned, cos_ref[own_rows, :], sin_ref[own_rows, :]).astype(BF16)

    pl.semaphore_wait(barrier, O - 1 + 3)

    def up_copy(d):
        return kv_copy(block(o, i, g, c), dev((o + d) % O, i, g, c), d)

    def relay_near(d, act):
        b = block(o - d, i, g, c)
        act(kv_copy(b, across, O + d))

        @pl.when((i == 0) | (d > 0))
        def _():
            act(kv_copy(b, beside, 2 * O + 2 * d))

        act(kv_copy(b, mate, 4 * O + 4 * d))

    def relay_far(d, act):
        b = block(o - d, i, 1 - g, c)

        @pl.when((i == 0) | (d > 0))
        def _():
            act(kv_copy(b, beside, 2 * O + 2 * d + 1))

        act(kv_copy(b, mate, 4 * O + 4 * d + 1))

    def relay_beside(d, act):
        act(kv_copy(block(o - d, 1 - i, g, c), mate, 4 * O + 4 * d + 2))
        act(kv_copy(block(o - d, 1 - i, 1 - g, c), mate, 4 * O + 4 * d + 3))

    def start(copy):
        copy.start()

    def sent(copy):
        copy.wait_send()

    def near(d):
        kv_wait(block(o - d, i, g, c))
        relay_near(d, start)

    def far(d):
        kv_wait(block(o - d, i, 1 - g, c))
        relay_far(d, start)

    def each(first, body):
        def run(d, carry):
            body(d)
            return carry

        lax.fori_loop(first, o + 1, run, 0)

    for d in range(1, O):

        @pl.when(o + d < O)
        def _(d=d):
            up_copy(d).start()

    relay_near(0, start)

    query = jnp.zeros((rows, dq.shape[1]), F32)
    for k in range(chunks):
        dq_loads[k].wait()
        query += dot(tokens[:, k * step : (k + 1) * step], dq[k * step : (k + 1) * step, :])
    ql[own_rows, :] = normed(query, qg_ref[...]).astype(BF16)

    def q_copy(t, target, index):
        part = ql.at[block_rows(t)]
        return pltpu.make_async_remote_copy(
            src_ref=part,
            dst_ref=part,
            send_sem=q_send.at[index],
            recv_sem=q_recv.at[t],
            device_id=target,
            device_id_type=MESH,
        )

    other = (1 - g) * 2 + c
    q_copies = [q_copy(tp, across, 0), q_copy(tp, mate, 1), q_copy(other, mate, 2)]
    q_copies[0].start()
    q_copies[1].start()

    far(0)
    each(1, near)
    up_loads[3].wait()
    uvt[...] = uv[...].T

    q_copy(other, mate, 2).wait_recv()
    q_copies[2].start()
    q_copy(g * 2 + 1 - c, mate, 0).wait_recv()
    q_copy((1 - g) * 2 + 1 - c, mate, 0).wait_recv()

    for copy in up_loads[:3]:
        copy.wait()
    plain = dot(ql[...], uq[...]).astype(BF16)
    turning = dot(ql[...], ur[...])
    low = lax.broadcasted_iota(jnp.int32, (span, LANES), 1) < ROPE
    for pair in range(heads // 2):
        both = turn(turning[:, pair * LANES : (pair + 1) * LANES], cos_ref[...], sin_ref[...])
        qh[2 * pair, :, NOPE:] = jnp.where(low, both, 0.0).astype(BF16)
        qh[2 * pair + 1, :, NOPE:] = jnp.where(low, pltpu.roll(both, ROPE, 1), 0.0).astype(BF16)
    for h in range(heads):
        qh[h, :, :NOPE] = plain[:, h * NOPE : (h + 1) * NOPE]
        best[h] = jnp.full(best.shape[1:], masked_score, F32)
        acc[h] = jnp.zeros(acc.shape[1:], F32)

    scale = (NOPE + ROPE) ** (-0.5) * log2e

    def attend(s, masked=False):
        part = pl.ds(pl.multiple_of(s * span, span), span)
        lat = kv[part, :rank]
        rot = kv[part, rank:]
        keys = dot(lat, uk[...]).astype(BF16)
        values = dot_nt(uvt[...], lat).astype(BF16)
        ones = jnp.ones((acc.shape[1] - VDIM, span), BF16)
        if masked:
            k_pos = lax.broadcasted_iota(jnp.int32, (span, span), 0)
            q_pos = lax.broadcasted_iota(jnp.int32, (span, span), 1)
            allowed = k_pos <= q_pos
        for h in range(heads):
            key = jnp.concatenate([keys[:, h * NOPE : (h + 1) * NOPE], rot], axis=1)
            value = jnp.concatenate([values[h * VDIM : (h + 1) * VDIM], ones], axis=0)
            scores = dot_nt(key, qh[h]) * scale
            if masked:
                scores = jnp.where(allowed, scores, masked_score)
            old = best[h][:1]
            new = jnp.maximum(old, jnp.max(scores, axis=0, keepdims=True))
            weights = jnp.exp2(scores - new).astype(BF16)
            acc[h] = acc[h] * jnp.exp2(old - new) + dot(value, weights)
            best[h] = jnp.broadcast_to(new, best.shape[1:])

    def own(d, masked=False):
        kv_wait(block(o - d, i, g, 1 - c))
        kv_wait(block(o - d, i, 1 - g, 1 - c))
        attend((o - d) * 2 + i, masked)

    def next_to(d):
        kv_wait(block(o - d, 1 - i, g, c))
        kv_wait(block(o - d, 1 - i, 1 - g, c))
        relay_beside(d, start)
        kv_wait(block(o - d, 1 - i, g, 1 - c))
        kv_wait(block(o - d, 1 - i, 1 - g, 1 - c))
        attend((o - d) * 2 + 1 - i)

    def column(d):
        @pl.when(d < o)
        def _():
            far(d + 1)

        own(d)

    @pl.when(o >= 1)
    def _():
        far(1)

    own(0, masked=True)
    pl.when(i == 1)(lambda: next_to(0))
    each(1, column)
    each(1, next_to)

    for h in range(heads):
        whole = acc[h]
        att[:, h * VDIM : (h + 1) * VDIM] = (whole[:VDIM] / whole[VDIM : VDIM + 1]).T.astype(BF16)

    ow_load.wait()
    width = ow.shape[1] // pieces

    def pair_copy(phase, j):
        return pltpu.make_async_remote_copy(
            src_ref=pair_out.at[phase, j],
            dst_ref=pair_in.at[phase, j],
            send_sem=pair_send.at[phase * pieces + j],
            recv_sem=pair_recv.at[phase * pieces + j],
            device_id=mate,
            device_id_type=MESH,
        )

    def cross_copy(j):
        return pltpu.make_async_remote_copy(
            src_ref=cross_out.at[j],
            dst_ref=cross_in.at[j],
            send_sem=cross_send.at[j],
            recv_sem=cross_recv.at[j],
            device_id=across,
            device_id_type=MESH,
        )

    def project(phase, group, j):
        top = att[block_rows(group * 2 + 1 - c), :]
        low_part = att[block_rows(group * 2 + c), :]
        part = dot(jnp.concatenate([top, low_part], axis=0), ow[:, j * width : (j + 1) * width])
        pair_out[phase, j] = part[:rows].astype(BF16)
        kept[phase, j] = part[rows:]
        pair_copy(phase, j).start()

    def cross(j):
        pair_copy(0, j).wait_recv()
        cross_out[j] = (kept[0, j] + pair_in[0, j].astype(F32)).astype(BF16)
        cross_copy(j).start()

    for j in range(pieces):
        project(0, 1 - g, j)
        if j >= 3:
            cross(j - 3)
    for j in range(pieces - 3, pieces):
        cross(j)
    for j in range(pieces):
        project(1, g, j)
    for j in range(pieces):
        pair_copy(1, j).wait_recv()
        cross_copy(j).wait_recv()
        total = kept[1, j] + pair_in[1, j].astype(F32) + cross_in[j].astype(F32)
        out_ref[:, j * width : (j + 1) * width] = total

    for d in range(1, O):

        @pl.when(o + d < O)
        def _(d=d):
            up_copy(d).wait_send()

    def drain(d, carry):
        relay_near(d, sent)
        relay_far(d, sent)

        @pl.when((i == 1) | (d > 0))
        def _():
            relay_beside(d, sent)

        return carry

    lax.fori_loop(0, o + 1, drain, 0)
    for copy in q_copies:
        copy.wait_send()
    for j in range(pieces):
        pair_copy(0, j).wait_send()
        pair_copy(1, j).wait_send()
        cross_copy(j).wait_send()


def solution(mesh):
    S, T = mesh.shape["sp"], mesh.shape["tp"]
    assert S % 2 == 0 and T == 4

    def local(tokens, dq, dl, dr, qg, lg, uq, ur, uk, uv, ow):
        rows, depth = tokens.shape
        span = rows * T
        heads = uk.shape[1] // NOPE
        width = ow.shape[1]
        rank = dl.shape[1]
        chunks, pieces = 4, 8
        inverse = np.float32(rope_base) ** (-np.arange(0, ROPE, 2, dtype=np.float32) / np.float32(ROPE))
        inverse = np.tile(inverse.astype(np.float64), LANES // (ROPE // 2))
        starts = np.arange(S)[:, None] * span * inverse
        steps = np.arange(span)[:, None] * inverse
        tables = [jnp.asarray(f(a), F32) for a in (starts, steps) for f in (np.cos, np.sin)]
        O = S // 2
        hbm = pl.BlockSpec(memory_space=pl.ANY)
        vmem = pl.BlockSpec(memory_space=pltpu.VMEM)
        dma = lambda n: pltpu.SemaphoreType.DMA((n,))
        like = lambda a: pltpu.VMEM(a.shape, a.dtype)
        total = pl.pallas_call(
            functools.partial(kernel, S, T, chunks, pieces),
            out_shape=jax.ShapeDtypeStruct((rows, width), F32),
            in_specs=[hbm, hbm, hbm, hbm, vmem, vmem, hbm, hbm, hbm, hbm, hbm, vmem, vmem, vmem, vmem],
            out_specs=vmem,
            scratch_shapes=[
                like(tokens),
                like(dq),
                like(dl),
                pltpu.VMEM(dr.shape[::-1], dr.dtype),
                like(uq),
                like(ur),
                like(uk),
                like(uv),
                like(ow),
                pltpu.VMEM((S * span, rank + LANES), BF16),
                pltpu.VMEM((span, dq.shape[1]), BF16),
                pltpu.VMEM((heads, span, NOPE + LANES), BF16),
                pltpu.VMEM((heads, VDIM + 16, span), F32),
                pltpu.VMEM((heads, 8, span), F32),
                pltpu.VMEM((span, heads * VDIM), BF16),
                pltpu.VMEM((2, pieces, rows, width // pieces), BF16),
                pltpu.VMEM((2, pieces, rows, width // pieces), BF16),
                pltpu.VMEM((2, pieces, rows, width // pieces), F32),
                pltpu.VMEM((pieces, rows, width // pieces), BF16),
                pltpu.VMEM((pieces, rows, width // pieces), BF16),
                pltpu.VMEM(uv.shape[::-1], BF16),
                pltpu.VMEM((span, LANES), F32),
                pltpu.VMEM((span, LANES), F32),
                dma(2 * chunks + 7),
                dma(8 * O),
                dma(S * T),
                dma(3),
                dma(T),
                dma(2 * pieces),
                dma(2 * pieces),
                dma(pieces),
                dma(pieces),
            ],
            compiler_params=pltpu.CompilerParams(
                collective_id=0, has_side_effects=True, vmem_limit_bytes=60 * 1024 * 1024
            ),
        )(
            tokens, dq, dl, dr.T, qg.reshape(1, -1), lg.reshape(1, -1),
            uq, ur, uk, uv, ow, *tables,
        )
        return total.astype(BF16)

    return jax.shard_map(
        local,
        mesh=mesh,
        in_specs=(
            P(("sp", "tp"), None),
            P(),
            P(),
            P(),
            P(),
            P(),
            P(None, "tp"),
            P(None, "tp"),
            P(None, "tp"),
            P(None, "tp"),
            P("tp", None),
        ),
        out_specs=P(("sp", "tp"), None),
        check_vma=False,
    )
```

```python
import functools

import jax
import jax.numpy as jnp
import numpy as np
from jax import lax
from jax.experimental import pallas as pl
from jax.experimental.pallas import tpu as pltpu
from jax.sharding import PartitionSpec as P

NOPE = 128
ROPE = 64
VDIM = 128
LANES = 128

rope_base = 500000.0
norm_eps = 1e-06
masked_score = -1e30
log2e = 1.4426950408889634

MESH = pl.DeviceIdType.MESH
F32 = jnp.float32
BF16 = jnp.bfloat16


def dot(a, b):
    return jnp.dot(a, b, preferred_element_type=F32)


def dot_nt(a, b):
    return lax.dot_general(a, b, (((1,), (1,)), ((), ())), preferred_element_type=F32)


def turn(v, cosine, sine):
    lane = lax.broadcasted_iota(jnp.int32, v.shape, 1)
    other = jnp.where(lane % ROPE < ROPE // 2, pltpu.roll(v, LANES - ROPE // 2, 1), pltpu.roll(v, ROPE // 2, 1))
    return v * cosine + other * sine


def normed(v, gain):
    return v * lax.rsqrt(jnp.mean(v * v, axis=-1, keepdims=True) + norm_eps) * gain


def kernel(
    S,
    T,
    chunks,
    pieces,
    tokens_hbm,
    dq_hbm,
    dl_hbm,
    dr_hbm,
    qg_ref,
    lg_ref,
    uq_hbm,
    ur_hbm,
    uk_hbm,
    uv_hbm,
    ow_hbm,
    base_cos,
    base_sin,
    row_cos,
    row_sin,
    out_ref,
    tokens,
    dq,
    dl,
    dr,
    uq,
    ur,
    uk,
    uv,
    ow,
    kv,
    ql,
    qh,
    acc,
    best,
    att,
    pair_out,
    pair_in,
    kept,
    cross_out,
    cross_in,
    uvt,
    cos_ref,
    sin_ref,
    load_sem,
    kv_send,
    kv_recv,
    q_send,
    q_recv,
    pair_send,
    pair_recv,
    cross_send,
    cross_recv,
):
    O = S // 2
    rows = tokens.shape[0]
    span = rows * T
    depth = tokens.shape[1]
    heads = qh.shape[0]
    rank = dl.shape[1]
    sp = lax.axis_index("sp")
    tp = lax.axis_index("tp")
    o, i = sp // 2, sp % 2
    g, c = tp // 2, tp % 2

    def dev(o_, i_, g_, c_):
        return {"sp": o_ * 2 + i_, "tp": g_ * 2 + c_}

    across = dev(o, i, 1 - g, c)
    beside = dev(o, 1 - i, g, c)
    mate = dev(o, i, g, 1 - c)

    step = depth // chunks
    loads = []

    def load(src, dst):
        copy = pltpu.make_async_copy(src, dst, load_sem.at[len(loads)])
        loads.append(copy)
        copy.start()
        return copy

    tok_load = load(tokens_hbm, tokens)
    dl_loads = [load(dl_hbm.at[pl.ds(k * step, step)], dl.at[pl.ds(k * step, step)]) for k in range(chunks)]
    dr_load = load(dr_hbm, dr)
    dq_loads = [load(dq_hbm.at[pl.ds(k * step, step)], dq.at[pl.ds(k * step, step)]) for k in range(chunks)]
    up_loads = [load(uq_hbm, uq), load(ur_hbm, ur), load(uk_hbm, uk), load(uv_hbm, uv)]
    ow_load = load(ow_hbm, ow)

    barrier = pltpu.get_barrier_semaphore()
    for d in range(1, O):
        pl.semaphore_signal(barrier, inc=1, device_id=dev((o + d) % O, i, g, c), device_id_type=MESH)
    for target in (across, beside, mate):
        pl.semaphore_signal(barrier, inc=1, device_id=target, device_id_type=MESH)

    def block(o_, i_, g_, c_):
        return (o_ * 2 + i_) * T + g_ * 2 + c_

    def block_rows(b):
        return pl.ds(pl.multiple_of(b * rows, rows), rows)

    def kv_copy(b, target, index):
        part = kv.at[block_rows(b)]
        return pltpu.make_async_remote_copy(
            src_ref=part,
            dst_ref=part,
            send_sem=kv_send.at[index],
            recv_sem=kv_recv.at[b],
            device_id=target,
            device_id_type=MESH,
        )

    def kv_wait(b):
        kv_copy(b, mate, 0).wait_recv()

    start_cos, start_sin = base_cos[pl.ds(sp, 1), :], base_sin[pl.ds(sp, 1), :]
    sign = jnp.where(lax.broadcasted_iota(jnp.int32, (1, LANES), 1) % ROPE < ROPE // 2, -1.0, 1.0)
    cos_ref[...] = start_cos * row_cos[...] - start_sin * row_sin[...]
    sin_ref[...] = (start_sin * row_cos[...] + start_cos * row_sin[...]) * sign

    tok_load.wait()
    latent = jnp.zeros((rows, rank), F32)
    for k in range(chunks):
        dl_loads[k].wait()
        latent += dot(tokens[:, k * step : (k + 1) * step], dl[k * step : (k + 1) * step, :])
    dr_load.wait()
    turned = dot_nt(tokens[...], dr[...])
    turned = jnp.concatenate([turned, jnp.zeros((rows, LANES - ROPE), F32)], axis=1)
    own_rows = pl.ds(pl.multiple_of(tp * rows, rows), rows)
    mine = block_rows(block(o, i, g, c))
    kv[mine, :rank] = normed(latent, lg_ref[...]).astype(BF16)
    kv[mine, rank:] = turn(turned, cos_ref[own_rows, :], sin_ref[own_rows, :]).astype(BF16)

    pl.semaphore_wait(barrier, O - 1 + 3)

    def up_copy(d):
        return kv_copy(block(o, i, g, c), dev((o + d) % O, i, g, c), d)

    def relay_near(d, act):
        b = block(o - d, i, g, c)
        act(kv_copy(b, across, O + d))

        @pl.when((i == 0) | (d > 0))
        def _():
            act(kv_copy(b, beside, 2 * O + 2 * d))

        act(kv_copy(b, mate, 4 * O + 4 * d))

    def relay_far(d, act):
        b = block(o - d, i, 1 - g, c)

        @pl.when(((i == 0) | (d > 0)) & (d < O - 1))
        def _():
            act(kv_copy(b, beside, 2 * O + 2 * d + 1))

        act(kv_copy(b, mate, 4 * O + 4 * d + 1))

    def relay_beside(d, act):
        b = block(o - d, 1 - i, g, c)

        @pl.when(d == O - 1)
        def _():
            act(kv_copy(b, across, 2 * O + 2 * d + 1))

        act(kv_copy(b, mate, 4 * O + 4 * d + 2))

    def relay_corner(d, act):
        act(kv_copy(block(o - d, 1 - i, 1 - g, c), mate, 4 * O + 4 * d + 3))

    def start(copy):
        copy.start()

    def sent(copy):
        copy.wait_send()

    def near(d):
        kv_wait(block(o - d, i, g, c))
        relay_near(d, start)

    def far(d):
        kv_wait(block(o - d, i, 1 - g, c))
        relay_far(d, start)

    def each(first, body):
        def run(d, carry):
            body(d)
            return carry

        lax.fori_loop(first, o + 1, run, 0)

    for d in range(1, O):

        @pl.when(o + d < O)
        def _(d=d):
            up_copy(d).start()

    relay_near(0, start)

    query = jnp.zeros((rows, dq.shape[1]), F32)
    for k in range(chunks):
        dq_loads[k].wait()
        query += dot(tokens[:, k * step : (k + 1) * step], dq[k * step : (k + 1) * step, :])
    ql[own_rows, :] = normed(query, qg_ref[...]).astype(BF16)

    def q_copy(t, target, index):
        part = ql.at[block_rows(t)]
        return pltpu.make_async_remote_copy(
            src_ref=part,
            dst_ref=part,
            send_sem=q_send.at[index],
            recv_sem=q_recv.at[t],
            device_id=target,
            device_id_type=MESH,
        )

    other = (1 - g) * 2 + c
    q_copies = [q_copy(tp, across, 0), q_copy(tp, mate, 1), q_copy(other, mate, 2)]
    q_copies[0].start()
    q_copies[1].start()

    far(0)
    each(1, near)
    up_loads[3].wait()
    uvt[...] = uv[...].T

    q_copy(other, mate, 2).wait_recv()
    q_copies[2].start()
    q_copy(g * 2 + 1 - c, mate, 0).wait_recv()
    q_copy((1 - g) * 2 + 1 - c, mate, 0).wait_recv()

    pl.when(o >= 1)(lambda: far(1))
    for copy in up_loads[:3]:
        copy.wait()
    plain = dot(ql[...], uq[...]).astype(BF16)
    turning = dot(ql[...], ur[...])
    low = lax.broadcasted_iota(jnp.int32, (span, LANES), 1) < ROPE
    for pair in range(heads // 2):
        both = turn(turning[:, pair * LANES : (pair + 1) * LANES], cos_ref[...], sin_ref[...])
        qh[2 * pair, :, NOPE:] = jnp.where(low, both, 0.0).astype(BF16)
        qh[2 * pair + 1, :, NOPE:] = jnp.where(low, pltpu.roll(both, ROPE, 1), 0.0).astype(BF16)
    for h in range(heads):
        qh[h, :, :NOPE] = plain[:, h * NOPE : (h + 1) * NOPE]
        best[h] = jnp.full(best.shape[1:], masked_score, F32)
        acc[h] = jnp.zeros(acc.shape[1:], F32)

    scale = (NOPE + ROPE) ** (-0.5) * log2e

    def attend(s, masked=False):
        part = pl.ds(pl.multiple_of(s * span, span), span)
        lat = kv[part, :rank]
        rot = kv[part, rank:]
        keys = dot(lat, uk[...]).astype(BF16)
        values = dot_nt(uvt[...], lat).astype(BF16)
        ones = jnp.ones((acc.shape[1] - VDIM, span), BF16)
        if masked:
            k_pos = lax.broadcasted_iota(jnp.int32, (span, span), 0)
            q_pos = lax.broadcasted_iota(jnp.int32, (span, span), 1)
            allowed = k_pos <= q_pos
        for h in range(heads):
            key = jnp.concatenate([keys[:, h * NOPE : (h + 1) * NOPE], rot], axis=1)
            value = jnp.concatenate([values[h * VDIM : (h + 1) * VDIM], ones], axis=0)
            scores = dot_nt(key, qh[h]) * scale
            if masked:
                scores = jnp.where(allowed, scores, masked_score)
            old = best[h][:1]
            new = jnp.maximum(old, jnp.max(scores, axis=0, keepdims=True))
            weights = jnp.exp2(scores - new).astype(BF16)
            acc[h] = acc[h] * jnp.exp2(old - new) + dot(value, weights)
            best[h] = jnp.broadcast_to(new, best.shape[1:])

    def own(d, masked=False):
        kv_wait(block(o - d, i, g, 1 - c))
        kv_wait(block(o - d, i, 1 - g, 1 - c))
        attend((o - d) * 2 + i, masked)

    def beside_in(d):
        kv_wait(block(o - d, 1 - i, g, c))
        relay_beside(d, start)

    def next_to(d):
        kv_wait(block(o - d, 1 - i, 1 - g, c))
        relay_corner(d, start)
        kv_wait(block(o - d, 1 - i, g, 1 - c))
        kv_wait(block(o - d, 1 - i, 1 - g, 1 - c))
        attend((o - d) * 2 + 1 - i)

    def column(d):
        pl.when(d + 3 <= o)(lambda: far(d + 3))
        own(d)

    pl.when(o >= 2)(lambda: far(2))
    own(0, masked=True)
    pl.when(o >= 3)(lambda: far(3))

    @pl.when(i == 1)
    def _():
        beside_in(0)
        next_to(0)

    each(1, beside_in)
    each(1, column)
    each(1, next_to)

    for h in range(heads):
        whole = acc[h]
        att[:, h * VDIM : (h + 1) * VDIM] = (whole[:VDIM] / whole[VDIM : VDIM + 1]).T.astype(BF16)

    ow_load.wait()
    width = ow.shape[1] // pieces
    lag = min(5, pieces)

    def pair_copy(phase, j):
        return pltpu.make_async_remote_copy(
            src_ref=pair_out.at[phase, j],
            dst_ref=pair_in.at[phase, j],
            send_sem=pair_send.at[phase * pieces + j],
            recv_sem=pair_recv.at[phase * pieces + j],
            device_id=mate,
            device_id_type=MESH,
        )

    def cross_copy(j):
        return pltpu.make_async_remote_copy(
            src_ref=cross_out.at[j],
            dst_ref=cross_in.at[j],
            send_sem=cross_send.at[j],
            recv_sem=cross_recv.at[j],
            device_id=across,
            device_id_type=MESH,
        )

    def project(phase, group, j):
        top = att[block_rows(group * 2 + 1 - c), :]
        low_part = att[block_rows(group * 2 + c), :]
        part = dot(jnp.concatenate([top, low_part], axis=0), ow[:, j * width : (j + 1) * width])
        pair_out[phase, j] = part[:rows].astype(BF16)
        kept[phase, j] = part[rows:]
        pair_copy(phase, j).start()

    def cross(j):
        pair_copy(0, j).wait_recv()
        cross_out[j] = (kept[0, j] + pair_in[0, j].astype(F32)).astype(BF16)
        cross_copy(j).start()

    for j in range(pieces):
        project(0, 1 - g, j)
        if j >= lag:
            cross(j - lag)
    for j in range(pieces - lag, pieces):
        cross(j)
    for j in range(pieces):
        project(1, g, j)
    for j in range(pieces):
        pair_copy(1, j).wait_recv()
        cross_copy(j).wait_recv()
        total = kept[1, j] + pair_in[1, j].astype(F32) + cross_in[j].astype(F32)
        out_ref[:, j * width : (j + 1) * width] = total

    for d in range(1, O):

        @pl.when(o + d < O)
        def _(d=d):
            up_copy(d).wait_send()

    def drain(d, carry):
        relay_near(d, sent)
        relay_far(d, sent)

        @pl.when((i == 1) | (d > 0))
        def _():
            relay_beside(d, sent)
            relay_corner(d, sent)

        return carry

    lax.fori_loop(0, o + 1, drain, 0)
    for copy in q_copies:
        copy.wait_send()
    for j in range(pieces):
        pair_copy(0, j).wait_send()
        pair_copy(1, j).wait_send()
        cross_copy(j).wait_send()


def solution(mesh):
    S, T = mesh.shape["sp"], mesh.shape["tp"]
    assert S % 2 == 0 and T == 4

    def local(tokens, dq, dl, dr, qg, lg, uq, ur, uk, uv, ow):
        rows, depth = tokens.shape
        span = rows * T
        heads = uk.shape[1] // NOPE
        width = ow.shape[1]
        rank = dl.shape[1]
        chunks, pieces = 4, 16
        inverse = np.float32(rope_base) ** (-np.arange(0, ROPE, 2, dtype=np.float32) / np.float32(ROPE))
        inverse = np.tile(inverse.astype(np.float64), LANES // (ROPE // 2))
        starts = np.arange(S)[:, None] * span * inverse
        steps = np.arange(span)[:, None] * inverse
        tables = [jnp.asarray(f(a), F32) for a in (starts, steps) for f in (np.cos, np.sin)]
        O = S // 2
        hbm = pl.BlockSpec(memory_space=pl.ANY)
        vmem = pl.BlockSpec(memory_space=pltpu.VMEM)
        dma = lambda n: pltpu.SemaphoreType.DMA((n,))
        like = lambda a: pltpu.VMEM(a.shape, a.dtype)
        total = pl.pallas_call(
            functools.partial(kernel, S, T, chunks, pieces),
            out_shape=jax.ShapeDtypeStruct((rows, width), F32),
            in_specs=[hbm, hbm, hbm, hbm, vmem, vmem, hbm, hbm, hbm, hbm, hbm, vmem, vmem, vmem, vmem],
            out_specs=vmem,
            scratch_shapes=[
                like(tokens),
                like(dq),
                like(dl),
                pltpu.VMEM(dr.shape[::-1], dr.dtype),
                like(uq),
                like(ur),
                like(uk),
                like(uv),
                like(ow),
                pltpu.VMEM((S * span, rank + LANES), BF16),
                pltpu.VMEM((span, dq.shape[1]), BF16),
                pltpu.VMEM((heads, span, NOPE + LANES), BF16),
                pltpu.VMEM((heads, VDIM + 16, span), F32),
                pltpu.VMEM((heads, 8, span), F32),
                pltpu.VMEM((span, heads * VDIM), BF16),
                pltpu.VMEM((2, pieces, rows, width // pieces), BF16),
                pltpu.VMEM((2, pieces, rows, width // pieces), BF16),
                pltpu.VMEM((2, pieces, rows, width // pieces), F32),
                pltpu.VMEM((pieces, rows, width // pieces), BF16),
                pltpu.VMEM((pieces, rows, width // pieces), BF16),
                pltpu.VMEM(uv.shape[::-1], BF16),
                pltpu.VMEM((span, LANES), F32),
                pltpu.VMEM((span, LANES), F32),
                dma(2 * chunks + 7),
                dma(8 * O),
                dma(S * T),
                dma(3),
                dma(T),
                dma(2 * pieces),
                dma(2 * pieces),
                dma(pieces),
                dma(pieces),
            ],
            compiler_params=pltpu.CompilerParams(
                collective_id=0, has_side_effects=True, vmem_limit_bytes=60 * 1024 * 1024
            ),
        )(
            tokens, dq, dl, dr.T, qg.reshape(1, -1), lg.reshape(1, -1),
            uq, ur, uk, uv, ow, *tables,
        )
        return total.astype(BF16)

    return jax.shard_map(
        local,
        mesh=mesh,
        in_specs=(
            P(("sp", "tp"), None),
            P(),
            P(),
            P(),
            P(),
            P(),
            P(None, "tp"),
            P(None, "tp"),
            P(None, "tp"),
            P(None, "tp"),
            P("tp", None),
        ),
        out_specs=P(("sp", "tp"), None),
        check_vma=False,
    )
```

```python
import functools

import jax
import jax.numpy as jnp
import numpy as np
from jax import lax
from jax.experimental import pallas as pl
from jax.experimental.pallas import tpu as pltpu
from jax.sharding import PartitionSpec as P

NOPE = 128
ROPE = 64
VDIM = 128
LANES = 128

rope_base = 500000.0
norm_eps = 1e-06
masked_score = -1e30
log2e = 1.4426950408889634

MESH = pl.DeviceIdType.MESH
F32 = jnp.float32
BF16 = jnp.bfloat16


def dot(a, b):
    return jnp.dot(a, b, preferred_element_type=F32)


def dot_nt(a, b):
    return lax.dot_general(a, b, (((1,), (1,)), ((), ())), preferred_element_type=F32)


def turn(v, cosine, sine):
    lane = lax.broadcasted_iota(jnp.int32, v.shape, 1)
    other = jnp.where(lane % ROPE < ROPE // 2, pltpu.roll(v, LANES - ROPE // 2, 1), pltpu.roll(v, ROPE // 2, 1))
    return v * cosine + other * sine


def normed(v, gain):
    return v * lax.rsqrt(jnp.mean(v * v, axis=-1, keepdims=True) + norm_eps) * gain


def kernel(
    S,
    T,
    chunks,
    pieces,
    tokens_hbm,
    dq_hbm,
    dl_hbm,
    dr_hbm,
    qg_ref,
    lg_ref,
    uq_hbm,
    ur_hbm,
    uk_hbm,
    uv_hbm,
    ow_hbm,
    base_cos,
    base_sin,
    row_cos,
    row_sin,
    out_ref,
    tokens,
    dq,
    dl,
    dr,
    uq,
    ur,
    uk,
    uv,
    ow,
    kv,
    ql,
    qh,
    acc,
    best,
    att,
    pair_out,
    pair_in,
    kept,
    cross_out,
    cross_in,
    uvt,
    first_keys,
    first_values,
    cos_ref,
    sin_ref,
    load_sem,
    kv_send,
    kv_recv,
    q_send,
    q_recv,
    pair_send,
    pair_recv,
    cross_send,
    cross_recv,
):
    O = S // 2
    rows = tokens.shape[0]
    span = rows * T
    depth = tokens.shape[1]
    heads = qh.shape[0]
    rank = dl.shape[1]
    sp = lax.axis_index("sp")
    tp = lax.axis_index("tp")
    o, i = sp // 2, sp % 2
    g, c = tp // 2, tp % 2

    def dev(o_, i_, g_, c_):
        return {"sp": o_ * 2 + i_, "tp": g_ * 2 + c_}

    across = dev(o, i, 1 - g, c)
    beside = dev(o, 1 - i, g, c)
    mate = dev(o, i, g, 1 - c)

    step = depth // chunks
    loads = []

    def load(src, dst):
        copy = pltpu.make_async_copy(src, dst, load_sem.at[len(loads)])
        loads.append(copy)
        copy.start()
        return copy

    tok_load = load(tokens_hbm, tokens)
    dl_loads = [load(dl_hbm.at[pl.ds(k * step, step)], dl.at[pl.ds(k * step, step)]) for k in range(chunks)]
    dr_load = load(dr_hbm, dr)
    dq_loads = [load(dq_hbm.at[pl.ds(k * step, step)], dq.at[pl.ds(k * step, step)]) for k in range(chunks)]
    up_loads = [load(uq_hbm, uq), load(ur_hbm, ur), load(uk_hbm, uk), load(uv_hbm, uv)]
    ow_load = load(ow_hbm, ow)

    barrier = pltpu.get_barrier_semaphore()
    for d in range(1, O):
        pl.semaphore_signal(barrier, inc=1, device_id=dev((o + d) % O, i, g, c), device_id_type=MESH)
    for target in (across, beside, mate):
        pl.semaphore_signal(barrier, inc=1, device_id=target, device_id_type=MESH)

    def block(o_, i_, g_, c_):
        return (o_ * 2 + i_) * T + g_ * 2 + c_

    def block_rows(b):
        return pl.ds(pl.multiple_of(b * rows, rows), rows)

    def kv_copy(b, target, index):
        part = kv.at[block_rows(b)]
        return pltpu.make_async_remote_copy(
            src_ref=part,
            dst_ref=part,
            send_sem=kv_send.at[index],
            recv_sem=kv_recv.at[b],
            device_id=target,
            device_id_type=MESH,
        )

    def kv_wait(b):
        kv_copy(b, mate, 0).wait_recv()

    start_cos, start_sin = base_cos[pl.ds(sp, 1), :], base_sin[pl.ds(sp, 1), :]
    sign = jnp.where(lax.broadcasted_iota(jnp.int32, (1, LANES), 1) % ROPE < ROPE // 2, -1.0, 1.0)
    cos_ref[...] = start_cos * row_cos[...] - start_sin * row_sin[...]
    sin_ref[...] = (start_sin * row_cos[...] + start_cos * row_sin[...]) * sign

    tok_load.wait()
    latent = jnp.zeros((rows, rank), F32)
    for k in range(chunks):
        dl_loads[k].wait()
        latent += dot(tokens[:, k * step : (k + 1) * step], dl[k * step : (k + 1) * step, :])
    dr_load.wait()
    turned = dot_nt(tokens[...], dr[...])
    turned = jnp.concatenate([turned, jnp.zeros((rows, LANES - ROPE), F32)], axis=1)
    own_rows = pl.ds(pl.multiple_of(tp * rows, rows), rows)
    mine = block_rows(block(o, i, g, c))
    kv[mine, :rank] = normed(latent, lg_ref[...]).astype(BF16)
    kv[mine, rank:] = turn(turned, cos_ref[own_rows, :], sin_ref[own_rows, :]).astype(BF16)

    pl.semaphore_wait(barrier, O - 1 + 3)

    def up_copy(d):
        return kv_copy(block(o, i, g, c), dev((o + d) % O, i, g, c), d)

    def relay_near(d, act):
        b = block(o - d, i, g, c)
        act(kv_copy(b, across, O + d))

        @pl.when((i == 0) | (d > 0))
        def _():
            act(kv_copy(b, beside, 2 * O + 2 * d))

        act(kv_copy(b, mate, 4 * O + 4 * d))

    def relay_far(d, act):
        b = block(o - d, i, 1 - g, c)

        @pl.when(((i == 0) | (d > 0)) & (d < O - 1))
        def _():
            act(kv_copy(b, beside, 2 * O + 2 * d + 1))

        act(kv_copy(b, mate, 4 * O + 4 * d + 1))

    def relay_beside(d, act):
        b = block(o - d, 1 - i, g, c)

        @pl.when(d == O - 1)
        def _():
            act(kv_copy(b, across, 2 * O + 2 * d + 1))

        act(kv_copy(b, mate, 4 * O + 4 * d + 2))

    def relay_corner(d, act):
        act(kv_copy(block(o - d, 1 - i, 1 - g, c), mate, 4 * O + 4 * d + 3))

    def start(copy):
        copy.start()

    def sent(copy):
        copy.wait_send()

    def near(d):
        kv_wait(block(o - d, i, g, c))
        relay_near(d, start)

    def far(d):
        kv_wait(block(o - d, i, 1 - g, c))
        relay_far(d, start)

    def beside_in(d):
        kv_wait(block(o - d, 1 - i, g, c))
        relay_beside(d, start)

    def corner_in(d):
        kv_wait(block(o - d, 1 - i, 1 - g, c))
        relay_corner(d, start)

    def each(first, body):
        def run(d, carry):
            body(d)
            return carry

        lax.fori_loop(first, o + 1, run, 0)

    for d in range(1, O):

        @pl.when(o + d < O)
        def _(d=d):
            up_copy(d).start()

    relay_near(0, start)

    query = jnp.zeros((rows, dq.shape[1]), F32)
    for k in range(chunks):
        dq_loads[k].wait()
        query += dot(tokens[:, k * step : (k + 1) * step], dq[k * step : (k + 1) * step, :])
    ql[own_rows, :] = normed(query, qg_ref[...]).astype(BF16)

    def q_copy(t, target, index):
        part = ql.at[block_rows(t)]
        return pltpu.make_async_remote_copy(
            src_ref=part,
            dst_ref=part,
            send_sem=q_send.at[index],
            recv_sem=q_recv.at[t],
            device_id=target,
            device_id_type=MESH,
        )

    other = (1 - g) * 2 + c
    q_copies = [q_copy(tp, across, 0), q_copy(tp, mate, 1), q_copy(other, mate, 2)]
    q_copies[0].start()
    q_copies[1].start()

    def kv_heads(s):
        part = pl.ds(pl.multiple_of(s * span, span), span)
        lat = kv[part, :rank]
        return dot(lat, uk[...]).astype(BF16), dot_nt(uvt[...], lat).astype(BF16)

    up_loads[2].wait()
    up_loads[3].wait()
    uvt[...] = uv[...].T
    far(0)
    pl.when(o >= 1)(lambda: near(1))
    kv_wait(block(o, i, g, 1 - c))
    kv_wait(block(o, i, 1 - g, 1 - c))
    first_keys[...], first_values[...] = kv_heads(sp)
    each(2, near)

    q_copy(other, mate, 2).wait_recv()
    q_copies[2].start()

    @pl.when(i == 1)
    def _():
        beside_in(0)
        corner_in(0)

    q_copy(g * 2 + 1 - c, mate, 0).wait_recv()
    q_copy((1 - g) * 2 + 1 - c, mate, 0).wait_recv()

    pl.when(o >= 1)(lambda: far(1))
    for copy in up_loads[:2]:
        copy.wait()
    scale = (NOPE + ROPE) ** (-0.5) * log2e
    plain = (dot(ql[...], uq[...]) * scale).astype(BF16)
    turning = dot(ql[...], ur[...]) * scale
    low = lax.broadcasted_iota(jnp.int32, (span, LANES), 1) < ROPE
    for pair in range(heads // 2):
        both = turn(turning[:, pair * LANES : (pair + 1) * LANES], cos_ref[...], sin_ref[...])
        qh[2 * pair, :, NOPE:] = jnp.where(low, both, 0.0).astype(BF16)
        qh[2 * pair + 1, :, NOPE:] = jnp.where(low, pltpu.roll(both, ROPE, 1), 0.0).astype(BF16)
    for h in range(heads):
        qh[h, :, :NOPE] = plain[:, h * NOPE : (h + 1) * NOPE]
        best[h] = jnp.full(best.shape[1:], masked_score, F32)
        acc[h] = jnp.zeros(acc.shape[1:], F32)

    def attend(s, masked=False):
        rot = kv[pl.ds(pl.multiple_of(s * span, span), span), rank:]
        keys, values = (first_keys[...], first_values[...]) if masked else kv_heads(s)
        ones = jnp.ones((acc.shape[1] - VDIM, span), BF16)
        if masked:
            k_pos = lax.broadcasted_iota(jnp.int32, (span, span), 0)
            q_pos = lax.broadcasted_iota(jnp.int32, (span, span), 1)
            allowed = k_pos <= q_pos

        def score(h):
            key = jnp.concatenate([keys[:, h * NOPE : (h + 1) * NOPE], rot], axis=1)
            return dot_nt(key, qh[h])

        ahead = score(0)
        for h in range(heads):
            scores = ahead
            if h + 1 < heads:
                ahead = score(h + 1)
            value = jnp.concatenate([values[h * VDIM : (h + 1) * VDIM], ones], axis=0)
            if masked:
                scores = jnp.where(allowed, scores, masked_score)
            old = best[h][:1]
            new = jnp.maximum(old, jnp.max(scores, axis=0, keepdims=True))
            weights = jnp.exp2(scores - new).astype(BF16)
            acc[h] = acc[h] * jnp.exp2(old - new) + dot(value, weights)
            best[h] = jnp.broadcast_to(new, best.shape[1:])

    def next_to(d):
        kv_wait(block(o - d, 1 - i, g, 1 - c))
        kv_wait(block(o - d, 1 - i, 1 - g, 1 - c))
        attend((o - d) * 2 + 1 - i)

    def column(d):
        pl.when(d + 3 <= o)(lambda: far(d + 3))
        kv_wait(block(o - d, i, g, 1 - c))
        kv_wait(block(o - d, i, 1 - g, 1 - c))
        attend((o - d) * 2 + i)
        corner_in(d)

    pl.when(o >= 2)(lambda: far(2))
    attend(sp, masked=True)
    pl.when(o >= 3)(lambda: far(3))
    each(1, beside_in)
    pl.when(i == 1)(lambda: next_to(0))
    each(1, column)
    each(1, next_to)

    for h in range(heads):
        whole = acc[h]
        att[:, h * VDIM : (h + 1) * VDIM] = (whole[:VDIM] / whole[VDIM : VDIM + 1]).T.astype(BF16)

    ow_load.wait()
    width = ow.shape[1] // pieces
    lag = min(3, pieces)

    def pair_copy(phase, j):
        return pltpu.make_async_remote_copy(
            src_ref=pair_out.at[phase, j],
            dst_ref=pair_in.at[phase, j],
            send_sem=pair_send.at[phase * pieces + j],
            recv_sem=pair_recv.at[phase * pieces + j],
            device_id=mate,
            device_id_type=MESH,
        )

    def cross_copy(j):
        return pltpu.make_async_remote_copy(
            src_ref=cross_out.at[j],
            dst_ref=cross_in.at[j],
            send_sem=cross_send.at[j],
            recv_sem=cross_recv.at[j],
            device_id=across,
            device_id_type=MESH,
        )

    def project(phase, group, j):
        top = att[block_rows(group * 2 + 1 - c), :]
        low_part = att[block_rows(group * 2 + c), :]
        part = dot(jnp.concatenate([top, low_part], axis=0), ow[:, j * width : (j + 1) * width])
        pair_out[phase, j] = part[:rows].astype(BF16)
        kept[phase, j] = part[rows:]
        pair_copy(phase, j).start()

    def cross(j):
        pair_copy(0, j).wait_recv()
        cross_out[j] = (kept[0, j] + pair_in[0, j].astype(F32)).astype(BF16)
        cross_copy(j).start()

    for j in range(pieces):
        project(0, 1 - g, j)
        if j >= lag:
            cross(j - lag)
    for j in range(pieces - lag, pieces):
        cross(j)
    for j in range(pieces):
        project(1, g, j)
    for j in range(pieces):
        pair_copy(1, j).wait_recv()
        cross_copy(j).wait_recv()
        total = kept[1, j] + pair_in[1, j].astype(F32) + cross_in[j].astype(F32)
        out_ref[:, j * width : (j + 1) * width] = total

    for d in range(1, O):

        @pl.when(o + d < O)
        def _(d=d):
            up_copy(d).wait_send()

    def drain(d, carry):
        relay_near(d, sent)
        relay_far(d, sent)

        @pl.when((i == 1) | (d > 0))
        def _():
            relay_beside(d, sent)
            relay_corner(d, sent)

        return carry

    lax.fori_loop(0, o + 1, drain, 0)
    for copy in q_copies:
        copy.wait_send()
    for j in range(pieces):
        pair_copy(0, j).wait_send()
        pair_copy(1, j).wait_send()
        cross_copy(j).wait_send()


def solution(mesh):
    S, T = mesh.shape["sp"], mesh.shape["tp"]
    assert S % 2 == 0 and T == 4

    def local(tokens, dq, dl, dr, qg, lg, uq, ur, uk, uv, ow):
        rows, depth = tokens.shape
        span = rows * T
        heads = uk.shape[1] // NOPE
        width = ow.shape[1]
        rank = dl.shape[1]
        chunks, pieces = 4, 8
        inverse = np.float32(rope_base) ** (-np.arange(0, ROPE, 2, dtype=np.float32) / np.float32(ROPE))
        inverse = np.tile(inverse.astype(np.float64), LANES // (ROPE // 2))
        starts = np.arange(S)[:, None] * span * inverse
        steps = np.arange(span)[:, None] * inverse
        tables = [jnp.asarray(f(a), F32) for a in (starts, steps) for f in (np.cos, np.sin)]
        O = S // 2
        hbm = pl.BlockSpec(memory_space=pl.ANY)
        vmem = pl.BlockSpec(memory_space=pltpu.VMEM)
        dma = lambda n: pltpu.SemaphoreType.DMA((n,))
        like = lambda a: pltpu.VMEM(a.shape, a.dtype)
        total = pl.pallas_call(
            functools.partial(kernel, S, T, chunks, pieces),
            out_shape=jax.ShapeDtypeStruct((rows, width), F32),
            in_specs=[hbm, hbm, hbm, hbm, vmem, vmem, hbm, hbm, hbm, hbm, hbm, vmem, vmem, vmem, vmem],
            out_specs=vmem,
            scratch_shapes=[
                like(tokens),
                like(dq),
                like(dl),
                pltpu.VMEM(dr.shape[::-1], dr.dtype),
                like(uq),
                like(ur),
                like(uk),
                like(uv),
                like(ow),
                pltpu.VMEM((S * span, rank + LANES), BF16),
                pltpu.VMEM((span, dq.shape[1]), BF16),
                pltpu.VMEM((heads, span, NOPE + LANES), BF16),
                pltpu.VMEM((heads, VDIM + 16, span), F32),
                pltpu.VMEM((heads, 8, span), F32),
                pltpu.VMEM((span, heads * VDIM), BF16),
                pltpu.VMEM((2, pieces, rows, width // pieces), BF16),
                pltpu.VMEM((2, pieces, rows, width // pieces), BF16),
                pltpu.VMEM((2, pieces, rows, width // pieces), F32),
                pltpu.VMEM((pieces, rows, width // pieces), BF16),
                pltpu.VMEM((pieces, rows, width // pieces), BF16),
                pltpu.VMEM(uv.shape[::-1], BF16),
                pltpu.VMEM((span, heads * NOPE), BF16),
                pltpu.VMEM((heads * VDIM, span), BF16),
                pltpu.VMEM((span, LANES), F32),
                pltpu.VMEM((span, LANES), F32),
                dma(2 * chunks + 7),
                dma(8 * O),
                dma(S * T),
                dma(3),
                dma(T),
                dma(2 * pieces),
                dma(2 * pieces),
                dma(pieces),
                dma(pieces),
            ],
            compiler_params=pltpu.CompilerParams(
                collective_id=0, has_side_effects=True, vmem_limit_bytes=60 * 1024 * 1024
            ),
        )(
            tokens, dq, dl, dr.T, qg.reshape(1, -1), lg.reshape(1, -1),
            uq, ur, uk, uv, ow, *tables,
        )
        return total.astype(BF16)

    return jax.shard_map(
        local,
        mesh=mesh,
        in_specs=(
            P(("sp", "tp"), None),
            P(),
            P(),
            P(),
            P(),
            P(),
            P(None, "tp"),
            P(None, "tp"),
            P(None, "tp"),
            P(None, "tp"),
            P("tp", None),
        ),
        out_specs=P(("sp", "tp"), None),
        check_vma=False,
    )
```

```python
import functools

import jax
import jax.numpy as jnp
import numpy as np
from jax import lax
from jax.experimental import pallas as pl
from jax.experimental.pallas import tpu as pltpu
from jax.sharding import PartitionSpec as P

NOPE = 128
ROPE = 64
VDIM = 128
LANES = 128

rope_base = 500000.0
norm_eps = 1e-06
masked_score = -1e30
log2e = 1.4426950408889634

MESH = pl.DeviceIdType.MESH
F32 = jnp.float32
BF16 = jnp.bfloat16


def dot(a, b):
    return jnp.dot(a, b, preferred_element_type=F32)


def dot_nt(a, b):
    return lax.dot_general(a, b, (((1,), (1,)), ((), ())), preferred_element_type=F32)


def turn(v, cosine, sine):
    lane = lax.broadcasted_iota(jnp.int32, v.shape, 1)
    other = jnp.where(lane % ROPE < ROPE // 2, pltpu.roll(v, LANES - ROPE // 2, 1), pltpu.roll(v, ROPE // 2, 1))
    return v * cosine + other * sine


def normed(v, gain):
    return v * lax.rsqrt(jnp.mean(v * v, axis=-1, keepdims=True) + norm_eps) * gain


def kernel(
    S,
    T,
    chunks,
    pieces,
    tokens_hbm,
    dq_hbm,
    dl_hbm,
    dr_hbm,
    qg_ref,
    lg_ref,
    uq_hbm,
    ur_hbm,
    uk_hbm,
    uv_hbm,
    ow_hbm,
    base_cos,
    base_sin,
    row_cos,
    row_sin,
    out_ref,
    tokens,
    dq,
    dl,
    dr,
    uq,
    ur,
    uk,
    uv,
    ow,
    kv,
    ql,
    qh,
    acc,
    best,
    att,
    pair_out,
    pair_in,
    kept,
    cross_out,
    cross_in,
    uvt,
    first_keys,
    first_values,
    cos_ref,
    sin_ref,
    load_sem,
    kv_send,
    kv_recv,
    q_send,
    q_recv,
    pair_send,
    pair_recv,
    cross_send,
    cross_recv,
):
    O = S // 2
    rows = tokens.shape[0]
    span = rows * T
    depth = tokens.shape[1]
    heads = qh.shape[0]
    rank = dl.shape[1]
    sp = lax.axis_index("sp")
    tp = lax.axis_index("tp")
    o, i = sp // 2, sp % 2
    g, c = tp // 2, tp % 2

    def dev(o_, i_, g_, c_):
        return {"sp": o_ * 2 + i_, "tp": g_ * 2 + c_}

    across = dev(o, i, 1 - g, c)
    beside = dev(o, 1 - i, g, c)
    mate = dev(o, i, g, 1 - c)

    step = depth // chunks
    loads = []

    def load(src, dst):
        copy = pltpu.make_async_copy(src, dst, load_sem.at[len(loads)])
        loads.append(copy)
        copy.start()
        return copy

    tok_load = load(tokens_hbm, tokens)
    dl_loads = [load(dl_hbm.at[pl.ds(k * step, step)], dl.at[pl.ds(k * step, step)]) for k in range(chunks)]
    dr_load = load(dr_hbm, dr)
    dq_loads = [load(dq_hbm.at[pl.ds(k * step, step)], dq.at[pl.ds(k * step, step)]) for k in range(chunks)]
    up_loads = [load(uq_hbm, uq), load(ur_hbm, ur), load(uk_hbm, uk), load(uv_hbm, uv)]
    ow_load = load(ow_hbm, ow)

    barrier = pltpu.get_barrier_semaphore()
    for d in range(1, O):
        pl.semaphore_signal(barrier, inc=1, device_id=dev((o + d) % O, i, g, c), device_id_type=MESH)
    for target in (across, beside, mate):
        pl.semaphore_signal(barrier, inc=1, device_id=target, device_id_type=MESH)

    def block(o_, i_, g_, c_):
        return (o_ * 2 + i_) * T + g_ * 2 + c_

    def block_rows(b):
        return pl.ds(pl.multiple_of(b * rows, rows), rows)

    def kv_copy(b, target, index):
        part = kv.at[block_rows(b)]
        return pltpu.make_async_remote_copy(
            src_ref=part,
            dst_ref=part,
            send_sem=kv_send.at[index],
            recv_sem=kv_recv.at[b],
            device_id=target,
            device_id_type=MESH,
        )

    def kv_wait(b):
        kv_copy(b, mate, 0).wait_recv()

    start_cos, start_sin = base_cos[pl.ds(sp, 1), :], base_sin[pl.ds(sp, 1), :]
    sign = jnp.where(lax.broadcasted_iota(jnp.int32, (1, LANES), 1) % ROPE < ROPE // 2, -1.0, 1.0)
    cos_ref[...] = start_cos * row_cos[...] - start_sin * row_sin[...]
    sin_ref[...] = (start_sin * row_cos[...] + start_cos * row_sin[...]) * sign

    tok_load.wait()
    latent = jnp.zeros((rows, rank), F32)
    for k in range(chunks):
        dl_loads[k].wait()
        latent += dot(tokens[:, k * step : (k + 1) * step], dl[k * step : (k + 1) * step, :])
    dr_load.wait()
    turned = dot_nt(tokens[...], dr[...])
    turned = jnp.concatenate([turned, jnp.zeros((rows, LANES - ROPE), F32)], axis=1)
    own_rows = pl.ds(pl.multiple_of(tp * rows, rows), rows)
    mine = block_rows(block(o, i, g, c))
    kv[mine, :rank] = normed(latent, lg_ref[...]).astype(BF16)
    kv[mine, rank:] = turn(turned, cos_ref[own_rows, :], sin_ref[own_rows, :]).astype(BF16)

    pl.semaphore_wait(barrier, O - 1 + 3)

    def up_copy(d):
        return kv_copy(block(o, i, g, c), dev((o + d) % O, i, g, c), d)

    def relay_near(d, act):
        b = block(o - d, i, g, c)
        act(kv_copy(b, across, O + d))

        @pl.when((i == 0) | (d > 0))
        def _():
            act(kv_copy(b, beside, 2 * O + 2 * d))

        act(kv_copy(b, mate, 4 * O + 4 * d))

    def relay_far(d, act):
        b = block(o - d, i, 1 - g, c)

        @pl.when(((i == 0) | (d > 0)) & (d < O - 1))
        def _():
            act(kv_copy(b, beside, 2 * O + 2 * d + 1))

        act(kv_copy(b, mate, 4 * O + 4 * d + 1))

    def relay_beside(d, act):
        b = block(o - d, 1 - i, g, c)

        @pl.when(d == O - 1)
        def _():
            act(kv_copy(b, across, 2 * O + 2 * d + 1))

        act(kv_copy(b, mate, 4 * O + 4 * d + 2))

    def relay_corner(d, act):
        act(kv_copy(block(o - d, 1 - i, 1 - g, c), mate, 4 * O + 4 * d + 3))

    def start(copy):
        copy.start()

    def sent(copy):
        copy.wait_send()

    def near(d):
        kv_wait(block(o - d, i, g, c))
        relay_near(d, start)

    def far(d):
        kv_wait(block(o - d, i, 1 - g, c))
        relay_far(d, start)

    def beside_in(d):
        kv_wait(block(o - d, 1 - i, g, c))
        relay_beside(d, start)

    def corner_in(d):
        kv_wait(block(o - d, 1 - i, 1 - g, c))
        relay_corner(d, start)

    def each(first, body):
        def run(d, carry):
            body(d)
            return carry

        lax.fori_loop(first, o + 1, run, 0)

    for d in range(1, O):

        @pl.when(o + d < O)
        def _(d=d):
            up_copy(d).start()

    relay_near(0, start)

    query = jnp.zeros((rows, dq.shape[1]), F32)
    for k in range(chunks):
        dq_loads[k].wait()
        query += dot(tokens[:, k * step : (k + 1) * step], dq[k * step : (k + 1) * step, :])
    ql[own_rows, :] = normed(query, qg_ref[...]).astype(BF16)

    def q_copy(t, target, index):
        part = ql.at[block_rows(t)]
        return pltpu.make_async_remote_copy(
            src_ref=part,
            dst_ref=part,
            send_sem=q_send.at[index],
            recv_sem=q_recv.at[t],
            device_id=target,
            device_id_type=MESH,
        )

    other = (1 - g) * 2 + c
    q_copies = [q_copy(tp, across, 0), q_copy(tp, mate, 1), q_copy(other, mate, 2)]
    q_copies[0].start()
    q_copies[1].start()

    def kv_heads(s):
        part = pl.ds(pl.multiple_of(s * span, span), span)
        lat = kv[part, :rank]
        return dot(lat, uk[...]).astype(BF16), dot_nt(uvt[...], lat).astype(BF16)

    up_loads[2].wait()
    up_loads[3].wait()
    uvt[...] = uv[...].T
    far(0)
    pl.when(o >= 1)(lambda: near(1))
    kv_wait(block(o, i, g, 1 - c))
    kv_wait(block(o, i, 1 - g, 1 - c))
    first_keys[...], first_values[...] = kv_heads(sp)
    each(2, near)

    q_copy(other, mate, 2).wait_recv()
    q_copies[2].start()

    @pl.when(i == 1)
    def _():
        beside_in(0)
        corner_in(0)

    q_copy(g * 2 + 1 - c, mate, 0).wait_recv()
    q_copy((1 - g) * 2 + 1 - c, mate, 0).wait_recv()

    pl.when(o >= 1)(lambda: far(1))
    for copy in up_loads[:2]:
        copy.wait()
    scale = (NOPE + ROPE) ** (-0.5) * log2e
    plain = (dot(ql[...], uq[...]) * scale).astype(BF16)
    turning = dot(ql[...], ur[...]) * scale
    low = lax.broadcasted_iota(jnp.int32, (span, LANES), 1) < ROPE
    for pair in range(heads // 2):
        both = turn(turning[:, pair * LANES : (pair + 1) * LANES], cos_ref[...], sin_ref[...])
        qh[2 * pair, :, NOPE:] = jnp.where(low, both, 0.0).astype(BF16)
        qh[2 * pair + 1, :, NOPE:] = jnp.where(low, pltpu.roll(both, ROPE, 1), 0.0).astype(BF16)
    for h in range(heads):
        qh[h, :, :NOPE] = plain[:, h * NOPE : (h + 1) * NOPE]
        best[h] = jnp.full(best.shape[1:], masked_score, F32)
        acc[h] = jnp.zeros(acc.shape[1:], F32)

    def attend(s, masked=False):
        rot = kv[pl.ds(pl.multiple_of(s * span, span), span), rank:]
        keys, values = (first_keys[...], first_values[...]) if masked else kv_heads(s)
        ones = jnp.ones((acc.shape[1] - VDIM, span), BF16)
        if masked:
            k_pos = lax.broadcasted_iota(jnp.int32, (span, span), 0)
            q_pos = lax.broadcasted_iota(jnp.int32, (span, span), 1)
            allowed = k_pos <= q_pos

        def score(h):
            key = jnp.concatenate([keys[:, h * NOPE : (h + 1) * NOPE], rot], axis=1)
            return dot_nt(key, qh[h])

        ahead = score(0)
        for h in range(heads):
            scores = ahead
            if h + 1 < heads:
                ahead = score(h + 1)
            value = jnp.concatenate([values[h * VDIM : (h + 1) * VDIM], ones], axis=0)
            if masked:
                scores = jnp.where(allowed, scores, masked_score)
            old = best[h][:1]
            new = jnp.maximum(old, jnp.max(scores, axis=0, keepdims=True))
            weights = jnp.exp2(scores - new).astype(BF16)
            acc[h] = acc[h] * jnp.exp2(old - new) + dot(value, weights)
            best[h] = jnp.broadcast_to(new, best.shape[1:])

    def next_to(d):
        kv_wait(block(o - d, 1 - i, g, 1 - c))
        kv_wait(block(o - d, 1 - i, 1 - g, 1 - c))
        attend((o - d) * 2 + 1 - i)

    def column(d):
        pl.when(d + 3 <= o)(lambda: far(d + 3))
        kv_wait(block(o - d, i, g, 1 - c))
        kv_wait(block(o - d, i, 1 - g, 1 - c))
        attend((o - d) * 2 + i)
        corner_in(d)

    attend(sp, masked=True)
    pl.when(o >= 2)(lambda: far(2))
    pl.when(i == 1)(lambda: next_to(0))
    pl.when(o >= 3)(lambda: far(3))
    each(1, beside_in)
    each(1, column)
    each(1, next_to)

    for h in range(heads):
        whole = acc[h]
        att[:, h * VDIM : (h + 1) * VDIM] = (whole[:VDIM] / whole[VDIM : VDIM + 1]).T.astype(BF16)

    ow_load.wait()
    width = ow.shape[1] // pieces
    lag = min(3, pieces)

    def pair_copy(phase, j):
        return pltpu.make_async_remote_copy(
            src_ref=pair_out.at[phase, j],
            dst_ref=pair_in.at[phase, j],
            send_sem=pair_send.at[phase * pieces + j],
            recv_sem=pair_recv.at[phase * pieces + j],
            device_id=mate,
            device_id_type=MESH,
        )

    def cross_copy(j):
        return pltpu.make_async_remote_copy(
            src_ref=cross_out.at[j],
            dst_ref=cross_in.at[j],
            send_sem=cross_send.at[j],
            recv_sem=cross_recv.at[j],
            device_id=across,
            device_id_type=MESH,
        )

    def project(phase, group, j):
        top = att[block_rows(group * 2 + 1 - c), :]
        low_part = att[block_rows(group * 2 + c), :]
        part = dot(jnp.concatenate([top, low_part], axis=0), ow[:, j * width : (j + 1) * width])
        pair_out[phase, j] = part[:rows].astype(BF16)
        kept[phase, j] = part[rows:]
        pair_copy(phase, j).start()

    def cross(j):
        pair_copy(0, j).wait_recv()
        cross_out[j] = (kept[0, j] + pair_in[0, j].astype(F32)).astype(BF16)
        cross_copy(j).start()

    for j in range(pieces):
        project(0, 1 - g, j)
        if j >= lag:
            cross(j - lag)
    for j in range(pieces - lag, pieces):
        cross(j)
    for j in range(pieces):
        project(1, g, j)
    for j in range(pieces):
        pair_copy(1, j).wait_recv()
        cross_copy(j).wait_recv()
        total = kept[1, j] + pair_in[1, j].astype(F32) + cross_in[j].astype(F32)
        out_ref[:, j * width : (j + 1) * width] = total

    for d in range(1, O):

        @pl.when(o + d < O)
        def _(d=d):
            up_copy(d).wait_send()

    def drain(d, carry):
        relay_near(d, sent)
        relay_far(d, sent)

        @pl.when((i == 1) | (d > 0))
        def _():
            relay_beside(d, sent)
            relay_corner(d, sent)

        return carry

    lax.fori_loop(0, o + 1, drain, 0)
    for copy in q_copies:
        copy.wait_send()
    for j in range(pieces):
        pair_copy(0, j).wait_send()
        pair_copy(1, j).wait_send()
        cross_copy(j).wait_send()


def solution(mesh):
    S, T = mesh.shape["sp"], mesh.shape["tp"]
    assert S % 2 == 0 and T == 4

    def local(tokens, dq, dl, dr, qg, lg, uq, ur, uk, uv, ow):
        rows, depth = tokens.shape
        span = rows * T
        heads = uk.shape[1] // NOPE
        width = ow.shape[1]
        rank = dl.shape[1]
        chunks, pieces = 4, 8
        inverse = np.float32(rope_base) ** (-np.arange(0, ROPE, 2, dtype=np.float32) / np.float32(ROPE))
        inverse = np.tile(inverse.astype(np.float64), LANES // (ROPE // 2))
        starts = np.arange(S)[:, None] * span * inverse
        steps = np.arange(span)[:, None] * inverse
        tables = [jnp.asarray(f(a), F32) for a in (starts, steps) for f in (np.cos, np.sin)]
        O = S // 2
        hbm = pl.BlockSpec(memory_space=pl.ANY)
        vmem = pl.BlockSpec(memory_space=pltpu.VMEM)
        dma = lambda n: pltpu.SemaphoreType.DMA((n,))
        like = lambda a: pltpu.VMEM(a.shape, a.dtype)
        total = pl.pallas_call(
            functools.partial(kernel, S, T, chunks, pieces),
            out_shape=jax.ShapeDtypeStruct((rows, width), F32),
            in_specs=[hbm, hbm, hbm, hbm, vmem, vmem, hbm, hbm, hbm, hbm, hbm, vmem, vmem, vmem, vmem],
            out_specs=vmem,
            scratch_shapes=[
                like(tokens),
                like(dq),
                like(dl),
                pltpu.VMEM(dr.shape[::-1], dr.dtype),
                like(uq),
                like(ur),
                like(uk),
                like(uv),
                like(ow),
                pltpu.VMEM((S * span, rank + LANES), BF16),
                pltpu.VMEM((span, dq.shape[1]), BF16),
                pltpu.VMEM((heads, span, NOPE + LANES), BF16),
                pltpu.VMEM((heads, VDIM + 16, span), F32),
                pltpu.VMEM((heads, 8, span), F32),
                pltpu.VMEM((span, heads * VDIM), BF16),
                pltpu.VMEM((2, pieces, rows, width // pieces), BF16),
                pltpu.VMEM((2, pieces, rows, width // pieces), BF16),
                pltpu.VMEM((2, pieces, rows, width // pieces), F32),
                pltpu.VMEM((pieces, rows, width // pieces), BF16),
                pltpu.VMEM((pieces, rows, width // pieces), BF16),
                pltpu.VMEM(uv.shape[::-1], BF16),
                pltpu.VMEM((span, heads * NOPE), BF16),
                pltpu.VMEM((heads * VDIM, span), BF16),
                pltpu.VMEM((span, LANES), F32),
                pltpu.VMEM((span, LANES), F32),
                dma(2 * chunks + 7),
                dma(8 * O),
                dma(S * T),
                dma(3),
                dma(T),
                dma(2 * pieces),
                dma(2 * pieces),
                dma(pieces),
                dma(pieces),
            ],
            compiler_params=pltpu.CompilerParams(
                collective_id=0, has_side_effects=True, vmem_limit_bytes=60 * 1024 * 1024
            ),
        )(
            tokens, dq, dl, dr.T, qg.reshape(1, -1), lg.reshape(1, -1),
            uq, ur, uk, uv, ow, *tables,
        )
        return total.astype(BF16)

    return jax.shard_map(
        local,
        mesh=mesh,
        in_specs=(
            P(("sp", "tp"), None),
            P(),
            P(),
            P(),
            P(),
            P(),
            P(None, "tp"),
            P(None, "tp"),
            P(None, "tp"),
            P(None, "tp"),
            P("tp", None),
        ),
        out_specs=P(("sp", "tp"), None),
        check_vma=False,
    )
```
